32 devices in a mesh: rep: 2 (over x), fs: 8 (over z, y), tp: 2 (over core).
Axes of the slice: x: 2, y: 2, z: 4, core: 2. Of those that a mesh axis runs over, the one named last changes fastest.
Arguments:
- mixed_input: bfloat16 [8192, 1024], P(('rep', 'fs', 'tp')), may hold values from -6 to 6
- project_weight: bfloat16 [1024, 1024], P(('fs', 'tp')), may hold values from -0.1875 to 0.1875
- norm_gain: float32 [1024], replicated, may hold values from 0.1 to 1.9
- up_weight: bfloat16 [1024, 4096], P('fs', 'tp'), may hold values from -0.1875 to 0.1875
- down_weight: bfloat16 [4096, 1024], P('tp', 'fs'), may hold values from -0.09375 to 0.09375
Outputs:
- mlp_output: bfloat16 [8192, 1024], P(('rep', 'fs', 'tp'))
The draws below stay inside these ranges and needn't reach their ends.
All inputs are finite; a program needn't handle non-finite values.
Results may differ from the reference program's by a relative error of at most 0.015.
Values may be sent and summed in bfloat16 or wider, within the bound.
A program may use at most 64 MiB of HBM per device.

```python
import jax
import jax.numpy as jnp
from jax import lax

D = 1024
MIX = 1024
FF = 4096
TOKENS = 8192
N_REP = 2
N_FS = 8


def block_levels(key, extent, shards, low, high):
    gain = 1.0
    for axis_at, blocks in shards:
        steps = jax.random.uniform(jax.random.fold_in(jax.random.fold_in(key, 6), axis_at), (blocks,), jnp.float32, low / len(shards), high / len(shards))
        gain = gain * jnp.repeat(jnp.exp(steps), extent[axis_at] // blocks).reshape((-1,) + (1,) * (len(extent) - 1 - axis_at))
    return gain


def gaussian(stream_key, extent, scale, bound, split=(), held_as=jnp.bfloat16):
    loudness = block_levels(stream_key, extent, split, -0.22, 0.18) if split else 1.0
    entries = jax.random.normal(stream_key, extent, jnp.float32) * scale * loudness
    return jnp.minimum(jnp.maximum(entries, -bound), bound).astype(held_as)


def setup_inputs(seed: int = 0) -> dict:
    splits = jax.random.split(jax.random.key(seed), 6)
    return {
        "mixed_input": gaussian(splits[0], (TOKENS, MIX), 1.0, 6.0, ((0, 32),)),
        "project_weight": gaussian(splits[1], (MIX, D), MIX ** -0.5, 0.1875, ((0, 16),)),
        "norm_gain": jnp.clip(1.0 + 0.18 * jax.random.normal(splits[2], (D,), jnp.float32), 0.1, 1.9),
        "up_weight": gaussian(splits[3], (D, FF), D ** -0.5, 0.1875, ((0, 8), (1, 2))),
        "down_weight": gaussian(splits[4], (FF, D), FF ** -0.5, 0.09375, ((0, 2), (1, 8))),
    }


epsilon = 1e-06

def reference(mixed_input, project_weight, norm_gain, up_weight, down_weight):
    block_count = N_REP * N_FS
    token_blocks = mixed_input.reshape(block_count, -1, mixed_input.shape[1])

    def block_output(row_block):
        projected = jnp.dot(row_block, project_weight, preferred_element_type=jnp.float32).astype(jnp.bfloat16)
        values = projected.astype(jnp.float32)
        scale = lax.rsqrt(lax.optimization_barrier(jnp.mean(values * values, axis=-1, keepdims=True)) + epsilon)
        normed = (values * scale * norm_gain.astype(jnp.float32)).astype(jnp.bfloat16)
        preact = jnp.dot(normed, up_weight, preferred_element_type=jnp.float32)
        hidden = jnp.square(jax.nn.relu(preact)).astype(jnp.bfloat16)
        return jnp.dot(hidden, down_weight, preferred_element_type=jnp.float32).astype(jnp.bfloat16)
    result = lax.map(block_output, token_blocks)
    return result.reshape(-1, down_weight.shape[1])
```

```python
import functools

import jax
import jax.numpy as jnp
from jax import lax
from jax.experimental import pallas as pl
from jax.experimental.pallas import tpu as pltpu
from jax.sharding import PartitionSpec as P

epsilon = 1e-06
MESH = pl.DeviceIdType.MESH


def kernel(R, F, T, ring_project, mixed_ref, project_ref, gain_ref, up_ref, down_ref, out_ref,
           mixed, project, up, down, hidden, own, outgoing, incoming,
           local_sem, mix_send, mix_recv, ring_send, ring_recv, pass_send, pass_recv,
           sum_send, sum_recv):
    G = R * T
    half_ring = F // 2
    r, f, t = lax.axis_index("rep"), lax.axis_index("fs"), lax.axis_index("tp")
    at = f // 2 + lax.rem(f, 2) * (F - 1 - 2 * (f // 2))

    def shard_at(position):
        position = lax.rem(position + 2 * F, F)
        back = position // half_ring
        return 2 * position * (1 - back) + back * (2 * (F - 1 - position) + 1)

    neighbour = (shard_at(at + 1), shard_at(at - 1))

    def owner(direction, distance):
        return shard_at(at - distance) if direction == 0 else shard_at(at + distance)

    def peer(k):
        return {"rep": lax.rem(r + k // T, R), "fs": f, "tp": lax.rem(t + lax.rem(k, T), T)}

    def seen_from(k):
        return lax.rem(R - k // T, R) * T + lax.rem(T - lax.rem(k, T), T)

    width = hidden.shape[-1]
    first = pl.multiple_of(r * width, width)
    if ring_project:
        rows = project_ref.shape[0]
    up_rows = up_ref.shape[0]

    def slices(tensor, who, h):
        if tensor == 0:
            n = project.shape[1] // 2
            place = pl.ds(pl.multiple_of((who * T + t) * rows, rows), rows)
            cols = pl.ds(h * n, n)
            return project_ref.at[:, cols], project.at[place, cols]
        if tensor == 1:
            n = up_rows // 2
            place = pl.ds(pl.multiple_of(who * up_rows + h * n, n), n)
            return up_ref.at[pl.ds(h * n, n), pl.ds(first, width)], up.at[place, :]
        n = width // 2
        source = down_ref.at[pl.ds(pl.multiple_of(r * width + h * n, n), n), :]
        return source, down.at[who, pl.ds(h * n, n), :]

    def hop(tensor, direction, distance, h):
        given, slot = slices(tensor, owner(direction, distance - 1), h)
        index = ((tensor * 2 + direction) * half_ring + distance - 1) * 2 + h
        return pltpu.make_async_remote_copy(
            src_ref=given if distance == 1 else slot,
            dst_ref=slot,
            send_sem=ring_send.at[index],
            recv_sem=ring_recv.at[index],
            device_id={"rep": r, "fs": neighbour[direction], "tp": t},
            device_id_type=MESH,
        )

    def arrived(tensor, direction, distance, h):
        index = ((tensor * 2 + direction) * half_ring + distance - 1) * 2 + h
        given, slot = slices(tensor, owner(direction, distance), h)
        pltpu.make_async_remote_copy(
            src_ref=slot, dst_ref=slot, send_sem=ring_send.at[index],
            recv_sem=ring_recv.at[index],
            device_id={"rep": r, "fs": neighbour[direction], "tp": t}, device_id_type=MESH,
        ).wait_recv()

    def halves(direction, distance):
        return (0, 1) if distance < half_ring else (direction,)

    started = []

    def step(tensor, distance):
        for h in (0, 1):
            for direction in (0, 1):
                if distance > 1:
                    arrived(tensor, direction, distance - 1, h)
                if h in halves(direction, distance):
                    copy = hop(tensor, direction, distance, h)
                    copy.start()
                    started.append(copy)

    def last(tensor):
        for direction in (0, 1):
            for h in halves(direction, half_ring):
                arrived(tensor, direction, half_ring, h)

    def owners(distance):
        if distance == 0:
            return ((0, f),)
        if distance == half_ring:
            return ((0, owner(0, distance)),)
        return ((0, owner(0, distance)), (1, owner(1, distance)))

    barrier = pltpu.get_barrier_semaphore()
    for direction in (0, 1):
        pl.semaphore_signal(barrier, inc=1, device_id={"rep": r, "fs": neighbour[direction], "tp": t},
                            device_id_type=MESH)
    for k in range(1, G):
        pl.semaphore_signal(barrier, inc=1, device_id=peer(k), device_id_type=MESH)
    pl.semaphore_wait(barrier, 2 + G - 1)

    if ring_project:
        step(0, 1)
    mixes = []
    for k in range(1, G):
        there = (R - k // T) % R * T + (T - k % T) % T
        copy = pltpu.make_async_remote_copy(
            src_ref=mixed_ref, dst_ref=mixed.at[there], send_sem=mix_send.at[k],
            recv_sem=mix_recv.at[there], device_id=peer(k), device_id_type=MESH)
        copy.start()
        mixes.append(copy)

    passes = []

    def pass_on(distance):
        for _, who in owners(distance):
            for dt in range(1, T):
                number = len(passes)
                place = project.at[pl.ds(pl.multiple_of((who * T + t) * rows, rows), rows), :]
                copy = pltpu.make_async_remote_copy(
                    src_ref=project_ref if distance == 0 else place, dst_ref=place,
                    send_sem=pass_send.at[number], recv_sem=pass_recv.at[number],
                    device_id=peer(dt), device_id_type=MESH)
                copy.start()
                passes.append((copy, who, dt))

    locals_ = [pltpu.make_async_copy(mixed_ref, mixed.at[0], local_sem.at[0])]
    for h in (0, 1):
        for tensor in (0, 1, 2) if ring_project else (1, 2):
            given, slot = slices(tensor, f, h)
            locals_.append(pltpu.make_async_copy(given, slot, local_sem.at[1 + 2 * tensor + h]))
    if not ring_project:
        locals_.append(pltpu.make_async_copy(project_ref, project, local_sem.at[1]))
    for copy in locals_:
        copy.start()
    if ring_project:
        pass_on(0)
        for distance in range(2, half_ring + 1):
            step(0, distance)
            pass_on(distance - 1)

    step(1, 1)
    if ring_project:
        last(0)
        pass_on(half_ring)
    step(1, 2) if half_ring > 1 else None
    for copy in locals_:
        copy.wait()
    if ring_project:
        for copy, who, dt in passes:
            copy.wait_recv()

    def norm_block(k):
        values = jnp.dot(mixed[k], project[...], preferred_element_type=jnp.float32)
        values = values.astype(jnp.bfloat16).astype(jnp.float32)
        scale = lax.rsqrt(jnp.mean(values * values, axis=-1, keepdims=True) + epsilon)
        mixed[k] = (values * scale * gain_ref[...]).astype(jnp.bfloat16)

    def norm_peer(k, carry):
        pltpu.make_async_copy(mixed.at[k], mixed.at[k], mix_recv.at[k]).wait()
        norm_block(k)
        return carry

    norm_block(0)
    split = max(G // 2, 1)
    lax.fori_loop(1, split, norm_peer, 0)
    for distance in range(3, half_ring + 1):
        step(1, distance)
    step(2, 1)
    lax.fori_loop(split, G, norm_peer, 0)
    last(1)

    def lift(k, carry):
        preact = jnp.dot(mixed[k], up[...], preferred_element_type=jnp.float32)
        hidden[k] = jnp.square(jnp.maximum(preact, 0.0)).astype(jnp.bfloat16)
        return carry

    lax.fori_loop(0, G, lift, 0)

    def sum_copy(k, who):
        there = seen_from(k)
        return pltpu.make_async_remote_copy(
            src_ref=outgoing.at[k, who], dst_ref=incoming.at[there, who],
            send_sem=sum_send.at[k, who], recv_sem=sum_recv.at[there, who],
            device_id=peer(k), device_id_type=MESH)

    def lower(who):
        def one(i, carry):
            k = G - i
            part = jnp.dot(hidden[k], down[who], preferred_element_type=jnp.float32)
            outgoing[k, who] = part.astype(jnp.bfloat16)
            sum_copy(k, who).start()
            return carry

        lax.fori_loop(1, G, one, 0)
        own[who] = jnp.dot(hidden[0], down[who], preferred_element_type=jnp.float32)

    for distance in range(2, half_ring + 1):
        step(2, distance)
        for _, who in owners(distance - 2):
            lower(who)
    for _, who in owners(half_ring - 1):
        lower(who)
    last(2)
    for _, who in owners(half_ring):
        lower(who)

    def settle(k, carry):
        for j in range(F):
            copy = sum_copy(k, j)
            copy.wait_send()
            pltpu.make_async_copy(incoming.at[k, j], incoming.at[k, j], sum_recv.at[k, j]).wait()
        return carry

    lax.fori_loop(1, G, settle, 0)
    w = own.shape[-1]
    for j in range(F):
        total = own[j]
        for k in range(1, G):
            total += incoming[k, j].astype(jnp.float32)
        out_ref[:, j * w:(j + 1) * w] = total.astype(jnp.bfloat16)
    for copy in started + mixes + [p[0] for p in passes]:
        copy.wait_send()


def local(R, F, T, mixed_input, project_weight, norm_gain, up_weight, down_weight):
    G = R * T
    tokens, mix = mixed_input.shape
    width = up_weight.shape[1] // R
    cols = down_weight.shape[1]
    model = project_weight.shape[1]
    ring_project = project_weight.shape[0] % 16 == 0
    if not ring_project:
        project_weight = lax.all_gather(project_weight, ("fs", "tp"), axis=0, tiled=True)
    hops = 3 * 2 * (F // 2) * 2
    dma = pltpu.SemaphoreType.DMA
    flops = 2 * G * tokens * (mix * model + 2 * model * width)
    return pl.pallas_call(
        functools.partial(kernel, R, F, T, ring_project),
        out_shape=jax.ShapeDtypeStruct((tokens, model), jnp.bfloat16),
        in_specs=[pl.BlockSpec(memory_space=pltpu.VMEM)] * 5,
        out_specs=pl.BlockSpec(memory_space=pltpu.VMEM),
        scratch_shapes=[
            pltpu.VMEM((G, tokens, mix), jnp.bfloat16),
            pltpu.VMEM((mix, model), jnp.bfloat16),
            pltpu.VMEM((model, width), jnp.bfloat16),
            pltpu.VMEM((F, width, cols), jnp.bfloat16),
            pltpu.VMEM((G, tokens, width), jnp.bfloat16),
            pltpu.VMEM((F, tokens, cols), jnp.float32),
            pltpu.VMEM((G, F, tokens, cols), jnp.bfloat16),
            pltpu.VMEM((G, F, tokens, cols), jnp.bfloat16),
            dma((8,)),
            dma((G,)), dma((G,)),
            dma((hops,)), dma((hops,)),
            dma((F * max(T - 1, 1),)), dma((F * max(T - 1, 1),)),
            dma((G, F)), dma((G, F)),
        ],
        compiler_params=pltpu.CompilerParams(
            collective_id=0, has_side_effects=True, vmem_limit_bytes=60 * 2 ** 20),
        cost_estimate=pl.CostEstimate(flops=flops, bytes_accessed=4 * 2 ** 20, transcendentals=0),
    )(mixed_input, project_weight, norm_gain.astype(jnp.float32).reshape(1, -1), up_weight, down_weight)


def solution(mesh):
    placed = (
        P(("rep", "fs", "tp"), None),
        P(("fs", "tp"), None),
        P(),
        P("fs", "tp"),
        P("tp", "fs"),
    )
    body = functools.partial(local, *(mesh.shape[name] for name in ("rep", "fs", "tp")))
    return jax.shard_map(
        body, mesh=mesh, in_specs=placed, out_specs=P(("rep", "fs", "tp"), None), check_vma=False
    )
```
